32 devices in a mesh: ra: 8 (over z, x), cb: 4 (over y, core).
Axes of the slice: x: 2, y: 2, z: 4, core: 2. Of those that a mesh axis runs over, the one named last changes fastest.
Arguments:
- inputs: bfloat16 [1536, 4096], P(None, 'ra'), may hold values from -12 to 12
- gate_weight: bfloat16 [2, 4096, 11264], P(None, 'ra', 'cb'), may hold values from -0.09375 to 0.09375
- up_weight: bfloat16 [2, 4096, 11264], P(None, 'ra', 'cb'), may hold values from -0.09375 to 0.09375
- down_weight: bfloat16 [2, 11264, 4096], P(None, 'cb', 'ra'), may hold values from -0.0546875 to 0.0546875
- norm_gain: float32 [2, 4096], P(None, 'ra'), may hold values from 0.05 to 8
- norm_shift: float32 [2, 4096], P(None, 'ra'), may hold values from -1.5 to 1.5
Outputs:
- outputs: bfloat16 [1536, 4096], P(None, 'ra')
The draws below stay inside these ranges and needn't reach their ends.
All inputs are finite; a program needn't handle non-finite values.
Results may differ from the reference program's by a relative error of at most 0.04.
Values may be sent and summed in bfloat16 or wider, within the bound.
A program may use at most 128 MiB of HBM per device.

```python
import jax
import jax.numpy as jnp
from jax import lax

D = 4096
FF = 11264
TOKENS = 1536
LAYERS = 2
N_RA = 8


def draw_inputs(key, part):
    key = jax.random.fold_in(key, 11)
    keys = jax.random.split(key, 3)
    groups = 32
    factor = jnp.exp(jax.random.uniform(keys[0], (1, groups), jnp.float32, jnp.log(0.3), jnp.log(3.0)))
    offset = jax.random.uniform(keys[1], (1, groups), jnp.float32, -1.0, 1.0)
    factor = jnp.repeat(factor, D // groups, axis=1)
    offset = jnp.repeat(offset, D // groups, axis=1)
    base = jax.random.normal(keys[2], (TOKENS, D), jnp.float32)
    return jnp.clip(base * factor + offset, -12.0, 12.0).astype(jnp.bfloat16)


def draw_norm_gain(key, part):
    key = jax.random.fold_in(key, 23)
    keys = jax.random.split(key, 2)
    groups = 32
    factor = jnp.exp(jax.random.uniform(keys[0], (LAYERS, groups), jnp.float32, jnp.log(0.35), jnp.log(3.0)))
    factor = jnp.repeat(factor, D // groups, axis=1)
    noise = jnp.clip(jax.random.normal(keys[1], (LAYERS, D), jnp.float32), -3.0, 3.0)
    return (factor * (1.0 + 0.18 * noise)).astype(jnp.float32)


def block_levels(stream_key, dims, pieces, low, high):
    level, own = 1.0, jax.random.fold_in(stream_key, 6)
    for axis_at, blocks in pieces:
        draws = jnp.exp(jax.random.uniform(jax.random.fold_in(own, axis_at), (blocks,), jnp.float32, low / len(pieces), high / len(pieces)))
        level = level * jnp.repeat(draws, dims[axis_at] // blocks).reshape([-1 if axis == axis_at else 1 for axis in range(len(dims))])
    return level


def scatter_about(key, shape, spread, most, pieces=(), dtype=jnp.bfloat16):
    loudness = block_levels(key, shape, pieces, -0.22, 0.18) if pieces else 1.0
    entries = jax.random.normal(key, shape, jnp.float32) * spread * loudness
    return jnp.minimum(jnp.maximum(entries, -most), most).astype(dtype)


def setup_inputs(seed: int = 0) -> dict:
    seeds = jax.random.split(jax.random.key(seed), 7)
    inputs = draw_inputs(jax.random.fold_in(seeds[6], 71), 0)
    gate_weight = scatter_about(seeds[1], (LAYERS, D, FF), D ** -0.5, 0.09375, ((1, 8), (2, 4)))
    up_weight = scatter_about(seeds[2], (LAYERS, D, FF), D ** -0.5, 0.09375, ((1, 8), (2, 4)))
    down_weight = scatter_about(seeds[3], (LAYERS, FF, D), FF ** -0.5, 0.0546875, ((1, 4), (2, 8)))
    norm_gain = draw_norm_gain(jax.random.fold_in(seeds[6], 71), 0)
    norm_shift = scatter_about(seeds[5], (LAYERS, D), 0.3, 1.5, ((1, 8),), jnp.float32)
    return {"inputs": inputs, "gate_weight": gate_weight, "up_weight": up_weight, "down_weight": down_weight, "norm_gain": norm_gain, "norm_shift": norm_shift}


RESIDUAL = 0.5
EPSILON = 1e-05

def block_products(stream, paired):
    width = D // N_RA
    total = jnp.zeros((stream.shape[0], paired.shape[1]), jnp.float32)
    for block_index in range(N_RA):
        start = block_index * width
        piece = jnp.dot(stream[:, start:start + width], paired[start:start + width], preferred_element_type=jnp.float32)
        rounded = lax.optimization_barrier(piece.astype(jnp.bfloat16))
        total = total + rounded.astype(jnp.float32)
    return total

def sublayer(stream, w_gate, w_up, w_down, gain_row, shift_row):
    columns = w_gate.shape[1]
    paired = jnp.concatenate((w_gate, w_up), axis=1)
    summed = block_products(stream, paired)
    hidden = (jax.nn.silu(summed[:, :columns]) * summed[:, columns:]).astype(jnp.bfloat16)
    branch = jnp.dot(hidden, w_down, preferred_element_type=jnp.float32)
    mixed_rows = RESIDUAL * stream.astype(jnp.float32) + branch
    mean_rows = lax.optimization_barrier(jnp.sum(mixed_rows, axis=1)) / D
    var_rows = lax.optimization_barrier(jnp.sum(mixed_rows * mixed_rows, axis=1)) / D - mean_rows * mean_rows
    normed = (mixed_rows - mean_rows[:, None]) * lax.rsqrt(var_rows + EPSILON)[:, None]
    return (normed * gain_row + shift_row).astype(jnp.bfloat16)

def reference(inputs, gate_weight, up_weight, down_weight, norm_gain, norm_shift):
    stream = inputs
    for layer_index in range(LAYERS):
        stream = sublayer(stream, gate_weight[layer_index], up_weight[layer_index], down_weight[layer_index], norm_gain[layer_index], norm_shift[layer_index])
    return stream
```

```python
import jax
import jax.numpy as jnp
from jax import lax
from jax.sharding import PartitionSpec as P

LAYERS = 2
RESIDUAL = 0.5
EPSILON = 1e-05
PAIR = 2
TOKEN_CHUNKS = 2
COLUMN_CHUNKS = 2
BF16 = jnp.bfloat16
F32 = jnp.float32


def dot(a, b):
    return jnp.dot(a, b, preferred_element_type=F32)


def axis_ring(total, stride, size):
    perm = []
    for i in range(total):
        at = (i // stride) % size
        perm.append((i, i + (((at + 1) % size) - at) * stride))
    return perm


def xor_perm(total, bit):
    return [(i, i ^ bit) for i in range(total)]


def swap(x, axis):
    return lax.ppermute(x, axis, xor_perm(lax.axis_size(axis), 1))


def part(x, at, size, dim=0):
    return lax.dynamic_slice_in_dim(x, at * size, size, dim)


def ring_reduce(block, axis, stride, size, me):
    perm = axis_ring(lax.axis_size(axis), stride, size)
    total = block(lax.rem(me + size - 1, size))
    for step in range(1, size):
        arrived = lax.ppermute(total.astype(BF16), axis, perm)
        total = arrived.astype(F32) + block(lax.rem(me + 2 * size - 1 - step, size))
    return total


def ring_gather(x, axis, stride, size, me):
    perm = axis_ring(lax.axis_size(axis), stride, size)
    rows = x.shape[0]
    whole = jnp.zeros((rows * size,) + x.shape[1:], x.dtype)
    whole = lax.dynamic_update_slice_in_dim(whole, x, me * rows, 0)
    for step in range(1, size):
        x = lax.ppermute(x, axis, perm)
        owner = lax.rem(me + size - step, size)
        whole = lax.dynamic_update_slice_in_dim(whole, x, owner * rows, 0)
    return whole


def swap_gather(x, axis, me):
    other = swap(x, axis)
    first = jnp.where(me == 0, x, other)
    second = jnp.where(me == 0, other, x)
    return jnp.concatenate((first, second), axis=0)


def sum_over_ra(stats):
    total = lax.axis_size("ra")
    if total & (total - 1):
        return lax.psum(stats, "ra")
    bit = 1
    while bit < total:
        stats = stats + lax.ppermute(stats, "ra", xor_perm(total, bit))
        bit *= 2
    return stats


def cuts_of(width):
    step = -(-width // COLUMN_CHUNKS)
    step = min(width, -(-step // 128) * 128)
    return [(s, min(step, width - s)) for s in range(0, width, step)]


def per_device(inputs, gate_weight, up_weight, down_weight, norm_gain, norm_shift):
    ra, cb = lax.axis_size("ra"), lax.axis_size("cb")
    r, c = lax.axis_index("ra"), lax.axis_index("cb")
    groups, rows_y = ra // PAIR, cb // 2
    q, g = lax.rem(r, PAIR), r // PAIR
    core, y = lax.rem(c, 2), c // 2
    tokens, width = inputs.shape
    full_width = width * ra
    columns = gate_weight.shape[2]
    half = columns // PAIR
    cuts = cuts_of(half)
    chunk = tokens // TOKEN_CHUNKS

    def weights_of(layer):
        kept, sent = q * half, (1 - q) * half
        pairs, downs = [], []
        for start, size in cuts:
            own = jnp.concatenate(
                [lax.dynamic_slice(w, (layer, 0, kept + start), (1, width, size))[0] for w in (gate_weight, up_weight)], axis=1
            )
            away = jnp.concatenate(
                [lax.dynamic_slice(w, (layer, 0, sent + start), (1, width, size))[0] for w in (gate_weight, up_weight)], axis=1
            )
            pairs.append((own, swap(away, "ra")))
        for start, size in cuts:
            own = lax.dynamic_slice(down_weight, (layer, kept + start, 0), (1, size, width))[0]
            away = lax.dynamic_slice(down_weight, (layer, sent + start, 0), (1, size, width))[0]
            downs.append((own, swap(away, "ra")))
        return pairs, downs

    streams = []
    for k in range(TOKEN_CHUNKS):
        own = inputs[k * chunk:(k + 1) * chunk]
        over = swap(part(own, core, chunk // 2), "ra")
        streams.append((own, swap_gather(over, "cb", core)))

    for layer in range(LAYERS):
        pairs, downs = weights_of(layer)
        last = layer == LAYERS - 1
        after = []
        for own, other in streams:
            block_rows = chunk // groups
            outs_own, outs_other = 0.0, 0.0
            for (w_own, w_other), (d_own, d_other) in zip(pairs, downs):
                size = d_own.shape[0]

                def block(at):
                    return dot(part(own, at, block_rows), w_own) + dot(part(other, at, block_rows), w_other)

                total = ring_reduce(block, "ra", PAIR, groups, g)
                hidden = (jax.nn.silu(total[:, :size]) * total[:, size:]).astype(BF16)
                hidden = ring_gather(hidden, "ra", PAIR, groups, g)
                outs_own = outs_own + dot(hidden, d_own)
                outs_other = outs_other + dot(hidden, d_other)
            out = jnp.concatenate((outs_own, outs_other), axis=1)
            out = part(out, core, chunk // 2) + swap(part(out, 1 - core, chunk // 2).astype(BF16), "cb").astype(F32)
            rows = chunk // cb
            out = ring_reduce(lambda at: part(out, at, rows), "cb", 2, rows_y, y)
            branch = out[:, :width] + swap(out[:, width:].astype(BF16), "ra").astype(F32)
            mine = lax.dynamic_slice_in_dim(own, core * (chunk // 2) + y * rows, rows, 0)
            mixed = RESIDUAL * mine.astype(F32) + branch
            stats = sum_over_ra(jnp.stack((jnp.sum(mixed, axis=1), jnp.sum(mixed * mixed, axis=1))))
            mean = stats[0] / full_width
            var = stats[1] / full_width - mean * mean
            normed = (mixed - mean[:, None]) * lax.rsqrt(var + EPSILON)[:, None]
            normed = (normed * norm_gain[layer] + norm_shift[layer]).astype(BF16)
            if not last:
                normed = jnp.concatenate((normed, swap(normed, "ra")), axis=1)
            whole = swap_gather(ring_gather(normed, "cb", 2, rows_y, y), "cb", core)
            after.append(whole if last else (whole[:, :width], whole[:, width:]))
        streams = after
    return jnp.concatenate(streams, axis=0)


def solution(mesh):
    return jax.shard_map(
        per_device,
        mesh=mesh,
        in_specs=(
            P(None, "ra"),
            P(None, "ra", "cb"),
            P(None, "ra", "cb"),
            P(None, "cb", "ra"),
            P(None, "ra"),
            P(None, "ra"),
        ),
        out_specs=P(None, "ra"),
        check_vma=False,
    )
```

```python
import jax
import jax.numpy as jnp
from jax import lax
from jax.sharding import PartitionSpec as P

LAYERS = 2
RESIDUAL = 0.5
EPSILON = 1e-05
PAIR = 2
TOKEN_CHUNKS = 3
COLUMN_CHUNKS = 2
BF16 = jnp.bfloat16
F32 = jnp.float32


def dot(a, b):
    return jnp.dot(a, b, preferred_element_type=F32)


def axis_ring(total, stride, size):
    perm = []
    for i in range(total):
        at = (i // stride) % size
        perm.append((i, i + (((at + 1) % size) - at) * stride))
    return perm


def xor_perm(total, bit):
    return [(i, i ^ bit) for i in range(total)]


def swap(x, axis):
    return lax.ppermute(x, axis, xor_perm(lax.axis_size(axis), 1))


def part(x, at, size, dim=0):
    return lax.dynamic_slice_in_dim(x, at * size, size, dim)


def ring_reduce(block, axis, stride, size, me):
    perm = axis_ring(lax.axis_size(axis), stride, size)
    total = block(lax.rem(me + size - 1, size))
    for step in range(1, size):
        arrived = lax.ppermute(total.astype(BF16), axis, perm)
        total = arrived.astype(F32) + block(lax.rem(me + 2 * size - 1 - step, size))
    return total


def ring_gather(x, axis, stride, size, me):
    perm = axis_ring(lax.axis_size(axis), stride, size)
    rows = x.shape[0]
    whole = jnp.zeros((rows * size,) + x.shape[1:], x.dtype)
    whole = lax.dynamic_update_slice_in_dim(whole, x, me * rows, 0)
    for step in range(1, size):
        x = lax.ppermute(x, axis, perm)
        owner = lax.rem(me + size - step, size)
        whole = lax.dynamic_update_slice_in_dim(whole, x, owner * rows, 0)
    return whole


def swap_gather(x, axis, me):
    other = swap(x, axis)
    first = jnp.where(me == 0, x, other)
    second = jnp.where(me == 0, other, x)
    return jnp.concatenate((first, second), axis=0)


def sum_over_ra(stats):
    total = lax.axis_size("ra")
    if total & (total - 1):
        return lax.psum(stats, "ra")
    bit = 1
    while bit < total:
        stats = stats + lax.ppermute(stats, "ra", xor_perm(total, bit))
        bit *= 2
    return stats


def cuts_of(width):
    step = -(-width // COLUMN_CHUNKS)
    step = min(width, -(-step // 128) * 128)
    return [(s, min(step, width - s)) for s in range(0, width, step)]


def per_device(inputs, gate_weight, up_weight, down_weight, norm_gain, norm_shift):
    ra, cb = lax.axis_size("ra"), lax.axis_size("cb")
    r, c = lax.axis_index("ra"), lax.axis_index("cb")
    groups, rows_y = ra // PAIR, cb // 2
    q, g = lax.rem(r, PAIR), r // PAIR
    core, y = lax.rem(c, 2), c // 2
    tokens, width = inputs.shape
    full_width = width * ra
    columns = gate_weight.shape[2]
    half = columns // PAIR
    cuts = cuts_of(half)
    chunk = tokens // TOKEN_CHUNKS

    queue = [None]

    def queued_swap(away):
        if queue[0] is not None:
            away, queue[0] = lax.optimization_barrier((away, queue[0]))
        queue[0] = swap(away, "ra")
        return queue[0]

    def weights_of(layer):
        kept, sent = q * half, (1 - q) * half
        pairs, downs = [], []
        for start, size in cuts:
            own = jnp.concatenate(
                [lax.dynamic_slice(w, (layer, 0, kept + start), (1, width, size))[0] for w in (gate_weight, up_weight)], axis=1
            )
            away = jnp.concatenate(
                [lax.dynamic_slice(w, (layer, 0, sent + start), (1, width, size))[0] for w in (gate_weight, up_weight)], axis=1
            )
            pairs.append((own, queued_swap(away)))
        for start, size in cuts:
            own = lax.dynamic_slice(down_weight, (layer, kept + start, 0), (1, size, width))[0]
            away = lax.dynamic_slice(down_weight, (layer, sent + start, 0), (1, size, width))[0]
            downs.append((own, queued_swap(away)))
        return pairs, downs

    streams = []
    for k in range(TOKEN_CHUNKS):
        own = inputs[k * chunk:(k + 1) * chunk]
        over = swap(part(own, core, chunk // 2), "ra")
        streams.append((own, swap_gather(over, "cb", core)))

    gate_open = None
    for layer in range(LAYERS):
        pairs, downs = weights_of(layer)
        last = layer == LAYERS - 1
        after = []
        for own, other in streams:
            block_rows = chunk // groups
            outs_own, outs_other = 0.0, 0.0
            if gate_open is not None:
                own, other, _ = lax.optimization_barrier((own, other, gate_open))
            opened = []
            for (w_own, w_other), (d_own, d_other) in zip(pairs, downs):
                size = d_own.shape[0]

                def block(at):
                    return dot(part(own, at, block_rows), w_own) + dot(part(other, at, block_rows), w_other)

                total = ring_reduce(block, "ra", PAIR, groups, g)
                hidden = (jax.nn.silu(total[:, :size]) * total[:, size:]).astype(BF16)
                opened.append(hidden)
                hidden = ring_gather(hidden, "ra", PAIR, groups, g)
                outs_own = outs_own + dot(hidden, d_own)
                outs_other = outs_other + dot(hidden, d_other)
            gate_open = tuple(h[:1] for h in opened)
            out = jnp.concatenate((outs_own, outs_other), axis=1)
            out = part(out, core, chunk // 2) + swap(part(out, 1 - core, chunk // 2).astype(BF16), "cb").astype(F32)
            rows = chunk // cb
            out = ring_reduce(lambda at: part(out, at, rows), "cb", 2, rows_y, y)
            branch = out[:, :width] + swap(out[:, width:].astype(BF16), "ra").astype(F32)
            mine = lax.dynamic_slice_in_dim(own, core * (chunk // 2) + y * rows, rows, 0)
            mixed = RESIDUAL * mine.astype(F32) + branch
            stats = sum_over_ra(jnp.stack((jnp.sum(mixed, axis=1), jnp.sum(mixed * mixed, axis=1))))
            mean = stats[0] / full_width
            var = stats[1] / full_width - mean * mean
            normed = (mixed - mean[:, None]) * lax.rsqrt(var + EPSILON)[:, None]
            normed = (normed * norm_gain[layer] + norm_shift[layer]).astype(BF16)
            if not last:
                normed = jnp.concatenate((normed, swap(normed, "ra")), axis=1)
            whole = swap_gather(ring_gather(normed, "cb", 2, rows_y, y), "cb", core)
            after.append(whole if last else (whole[:, :width], whole[:, width:]))
        streams = after
    return jnp.concatenate(streams, axis=0)


def solution(mesh):
    return jax.shard_map(
        per_device,
        mesh=mesh,
        in_specs=(
            P(None, "ra"),
            P(None, "ra", "cb"),
            P(None, "ra", "cb"),
            P(None, "cb", "ra"),
            P(None, "ra"),
            P(None, "ra"),
        ),
        out_specs=P(None, "ra"),
        check_vma=False,
    )
```
